128 devices in a mesh: fs: 16 (over z, x), tp: 8 (over y, core).
Axes of the slice: x: 4, y: 4, z: 4, core: 2. Of those that a mesh axis runs over, the one named last changes fastest.
Arguments:
- stream: bfloat16 [8192, 2048], P('fs', 'tp'), may hold values from -6 to 6
- gain_mix: float32 [2048], replicated, may hold values from 0.1 to 1.9
- pool_weight: bfloat16 [4, 512, 512], P(None, 'fs', 'tp'), may hold values from -0.25 to 0.25
- pool_gain: float32 [2048], replicated, may hold values from 0.1 to 1.9
- gain_ffn: float32 [2048], replicated, may hold values from 0.1 to 1.9
- gate_weight: bfloat16 [2048, 5632], P('fs', 'tp'), may hold values from -0.125 to 0.125
- up_weight: bfloat16 [2048, 5632], P('fs', 'tp'), may hold values from -0.125 to 0.125
- gate_taps: float32 [3, 5632], replicated, may hold values from -2.5 to 2.5
- up_taps: float32 [3, 5632], replicated, may hold values from -2.5 to 2.5
- down_weight: bfloat16 [5632, 2048], P('tp', 'fs'), may hold values from -0.078125 to 0.078125
Outputs:
- layer_out: bfloat16 [8192, 2048], P('fs', 'tp')
The draws below stay inside these ranges and needn't reach their ends.
All inputs are finite; a program needn't handle non-finite values.
Results may differ from the reference program's by a relative error of at most 0.01.
Values may be sent and summed in bfloat16 or wider, within the bound.
No kernel may reach another device: no remote copies, remote signals or barrier semaphores. Data moves between devices by JAX's collectives and lax.ppermute only.
A program may use at most 64 MiB of HBM per device.

```python
import jax
import jax.numpy as jnp
from jax import lax

D = 2048
G = 4
FF = 5632
TAPS = 3
LEN = 128
CG = 512
TOKENS = 8192


def level_of(own_key, dims, cuts, smallest, top_value):
    loudness, own = 1.0, jax.random.fold_in(own_key, 6)
    for axis_at, blocks in cuts:
        heights = jnp.exp(jax.random.uniform(jax.random.fold_in(own, axis_at), (blocks,), jnp.float32, smallest / len(cuts), top_value / len(cuts)))
        loudness = loudness * jnp.repeat(heights, dims[axis_at] // blocks).reshape([-1 if axis == axis_at else 1 for axis in range(len(dims))])
    return loudness


def scatter_about(own_key, shape, scale, limit, split=(), held_as=jnp.bfloat16):
    values = scale * jax.random.normal(own_key, shape, jnp.float32)
    if split:
        values = values * level_of(own_key, shape, split, -0.22, 0.18)
    return jnp.clip(values, -limit, limit).astype(held_as)


def setup_inputs(seed: int = 0) -> dict:
    streams_of = jax.random.split(jax.random.key(seed), 11)
    stream = scatter_about(streams_of[0], (TOKENS, D), 1.0, 6.0, ((0, 16), (1, 8)))
    gain_mix = jnp.clip(1.0 + 0.18 * jax.random.normal(streams_of[1], (D,), jnp.float32), 0.1, 1.9)
    pool_weight = scatter_about(streams_of[2], (G, CG, CG), CG ** -0.5, 0.25, ((1, 16), (2, 8)))
    pool_gain = jnp.clip(1.0 + 0.18 * jax.random.normal(streams_of[3], (D,), jnp.float32), 0.1, 1.9)
    gain_ffn = jnp.clip(1.0 + 0.18 * jax.random.normal(streams_of[4], (D,), jnp.float32), 0.1, 1.9)
    gate_weight = scatter_about(streams_of[5], (D, FF), D ** -0.5, 0.125, ((0, 16), (1, 8)))
    up_weight = scatter_about(streams_of[6], (D, FF), D ** -0.5, 0.125, ((0, 16), (1, 8)))
    gate_taps = scatter_about(streams_of[7], (TAPS, FF), 0.577, 2.5, (), jnp.float32)
    up_taps = scatter_about(streams_of[8], (TAPS, FF), 0.577, 2.5, (), jnp.float32)
    down_weight = scatter_about(streams_of[9], (FF, D), FF ** -0.5, 0.078125, ((0, 8), (1, 16)))
    return dict(stream=stream, gain_mix=gain_mix, pool_weight=pool_weight, pool_gain=pool_gain, gain_ffn=gain_ffn, gate_weight=gate_weight, up_weight=up_weight, gate_taps=gate_taps, up_taps=up_taps, down_weight=down_weight)


epsilon = 1e-06

def rms_norm(values, scales):
    return values * lax.rsqrt(lax.optimization_barrier(jnp.mean(values * values, axis=-1, keepdims=True)) + epsilon) * scales

def delayed(values, amount):
    return jnp.pad(values, ((0, 0), (amount, 0), (0, 0)))[:, :values.shape[1]]

def pool_less(values):
    channels = values.shape[2]
    group_id = jnp.arange(channels) % 4
    partials = [values]
    running = values
    for amount in (1, 2, 4, 8):
        running = running + delayed(running, amount)
        partials.append(running)
    picked = jnp.where(group_id == 0, partials[1], jnp.where(group_id == 1, partials[2], jnp.where(group_id == 2, partials[3], partials[4])))
    extent = jnp.where(group_id == 0, 2.0, jnp.where(group_id == 1, 4.0, jnp.where(group_id == 2, 8.0, 16.0)))
    position = jnp.arange(values.shape[1]).astype(jnp.float32)[:, None] + 1.0
    divisor = jnp.minimum(position, extent[None, :])
    return picked / divisor[None] - values

def causal_taps(values, kernel):
    reach = kernel.shape[0]
    length = values.shape[1]
    padded = jnp.pad(values, ((0, 0), (reach - 1, 0), (0, 0)))
    running = padded[:, 0:length] * kernel[0]
    for shift_by in range(1, reach):
        running = running + padded[:, shift_by:shift_by + length] * kernel[shift_by]
    return running

def reference(stream, gain_mix, pool_weight, pool_gain, gain_ffn, gate_weight, up_weight, gate_taps, up_taps, down_weight):
    tok_rows = stream.shape[0]
    seq_count = tok_rows // LEN
    normed = lax.optimization_barrier(rms_norm(stream.astype(jnp.float32), gain_mix).astype(jnp.bfloat16))
    pooled = pool_less(normed.astype(jnp.float32).reshape(seq_count, LEN, D)).astype(jnp.bfloat16)
    pooled = pooled.reshape(tok_rows, CG, G)
    mixer = jnp.einsum('tcg,gce->teg', pooled.astype(jnp.float32), pool_weight.astype(jnp.float32)).reshape(tok_rows, D) * pool_gain
    middle = lax.optimization_barrier((stream.astype(jnp.float32) + mixer).astype(jnp.bfloat16))
    normed_ffn = rms_norm(middle.astype(jnp.float32), gain_ffn).astype(jnp.bfloat16)
    gate_proj = lax.optimization_barrier(jnp.dot(normed_ffn, gate_weight, preferred_element_type=jnp.float32).astype(jnp.bfloat16))
    value_proj = lax.optimization_barrier(jnp.dot(normed_ffn, up_weight, preferred_element_type=jnp.float32).astype(jnp.bfloat16))
    gate_conv = causal_taps(gate_proj.astype(jnp.float32).reshape(seq_count, LEN, FF), gate_taps)
    value_conv = causal_taps(value_proj.astype(jnp.float32).reshape(seq_count, LEN, FF), up_taps)
    hidden = (jax.nn.silu(gate_conv) * value_conv).astype(jnp.bfloat16).reshape(tok_rows, FF)
    return jnp.dot(hidden, down_weight, preferred_element_type=jnp.float32).astype(jnp.bfloat16)
```

```python
import jax
import jax.numpy as jnp
import numpy as np
from jax import lax
from jax.experimental import pallas as pl
from jax.experimental.pallas import tpu as pltpu
from jax.sharding import PartitionSpec as P

LEN = 128
EPS = 1e-06
BF = jnp.bfloat16
F32 = jnp.float32
AXES = ("fs", "tp")


def pair(kind, v):
    return v ^ 1 if kind == 0 else 3 - v


DIMS = {
    (0, 0): (("x", 0), ("z", 0), ("x", 1), ("z", 1)),
    (0, 1): (("z", 0), ("x", 0), ("z", 1), ("x", 1)),
    (1, 0): (("x", 1), ("z", 1), ("x", 0), ("z", 0)),
    (1, 1): (("z", 1), ("x", 1), ("z", 0), ("x", 0)),
}
YDIMS = {0: (0, 1), 1: (1, 0)}


def hop(step, z, x):
    axis, kind = step
    return (pair(kind, z), x) if axis == "z" else (z, pair(kind, x))


def number(z, x, y, c):
    return (z * 4 + x) * 8 + y * 2 + c


def everyone():
    for z in range(4):
        for x in range(4):
            for y in range(4):
                for c in range(2):
                    yield z, x, y, c


def weight_perm(half, step):
    out = []
    for z, x, y, c in everyone():
        to = hop(DIMS[half, c][step], z, x)
        out.append((number(z, x, y, c), number(*to, y, c)))
    return out


def column_perm(step):
    return [
        (number(z, x, y, c), number(z, x, pair(YDIMS[c][step], y), c)) for z, x, y, c in everyone()
    ]


def core_perm():
    return [(number(z, x, y, c), number(z, x, y, 1 - c)) for z, x, y, c in everyone()]


def order_of_four(half, c, z, x):
    first, second = DIMS[half, c][:2]
    spots = [(z, x), hop(first, z, x), hop(second, z, x), hop(first, *hop(second, z, x))]
    return [a * 4 + b for a, b in spots]


def order_of_all(half, c, z, x):
    third, fourth = DIMS[half, c][2:]
    out = []
    for spot in ((z, x), hop(third, z, x), hop(fourth, z, x), hop(third, *hop(fourth, z, x))):
        out += order_of_four(half, c, *spot)
    return out


def order_of_columns(c, y):
    a, b = YDIMS[c]
    return [y, pair(a, y), pair(b, y), pair(a, pair(b, y))]


def tables():
    rows = []
    for z, x, y, c in everyone():
        row = order_of_all(0, c, z, x) + order_of_all(1, c, z, x)
        for core in (c, 1 - c):
            got = order_of_columns(core, y)
            row += [got.index(v) for v in range(4)]
        a, b = YDIMS[c]
        row += [pair(a, y), pair(b, pair(a, y)), y, pair(b, y), c, y, 0, 0]
        rows.append(row)
    return np.array(rows, np.int32)


SLOT = 32
LAST = 40
CORE = 44

VMEM = pl.BlockSpec(memory_space=pltpu.VMEM)
SMEM = pl.BlockSpec(memory_space=pltpu.SMEM)


def call(kernel, name, outs, n_in, table=False, scratch=(), flops=0):
    return pl.pallas_call(
        kernel,
        name=name,
        out_shape=[jax.ShapeDtypeStruct(s, d) for s, d in outs],
        in_specs=([SMEM] if table else []) + [VMEM] * n_in,
        out_specs=[VMEM] * len(outs),
        scratch_shapes=list(scratch),
        compiler_params=pltpu.CompilerParams(vmem_limit_bytes=48 * 1024 * 1024),
        cost_estimate=pl.CostEstimate(flops=flops, bytes_accessed=1 << 20, transcendentals=0),
    )


def send(value, perm):
    return lax.ppermute(value, AXES, perm)


def first_pack(g, u, d, p, a, b, spread):
    a[0:704, :] = g[...]
    a[704:1088, :] = d[0:384, :]
    b[0:704, :] = u[...]
    b[704:1024, :] = d[384:704, :]
    for k in range(2):
        both = jnp.concatenate([p[2 * k].astype(F32), p[2 * k + 1].astype(F32)], axis=1)
        for i in range(16):
            spread[i, k] = both.astype(BF)


def pack_two(a, ra, b, rb, oa, ob):
    oa[0] = a[...]
    oa[1] = ra[...]
    ob[0] = b[...]
    ob[1] = rb[...]


def pack_four(a, ra, b, rb, ga, da, gb, db):
    for src, at in ((a, 0), (ra, 2)):
        for i in range(2):
            ga[at + i] = src[i, 0:704, :]
            da[at + i] = src[i, 704:1088, :]
    for src, at in ((b, 0), (rb, 2)):
        for i in range(2):
            gb[at + i] = src[i, 0:704, :]
            db[at + i] = src[i, 704:1024, :]


def column_pack(stream, pool, q):
    q[0] = stream[:, 0:128]
    q[1] = stream[:, 128:256]
    for f in range(16):
        for k in range(2):
            q[2 + k, 32 * f : 32 * f + 32, :] = pool[f, k]


def column_two(q, r, o):
    o[0] = q[...]
    o[1] = r[...]


def column_four(q2, r2, o):
    o[0:2] = q2[...]
    o[2:4] = r2[...]


def mix_kernel(
    tab, own, other, gain_mix, pool_gain, gain_ffn, out, xs, ns, ng, pw, hi, lo, perm, back
):
    core = tab[CORE]
    first = core == 0
    rows = lax.broadcasted_iota(jnp.int32, (512, 512), 0)
    cols = lax.broadcasted_iota(jnp.int32, (512, 512), 1)
    perm[...] = jnp.where((rows % 4) * 128 + rows // 4 == cols, 1.0, 0.0).astype(BF)
    back[...] = jnp.where((cols % 4) * 128 + cols // 4 == rows, 1.0, 0.0).astype(BF)
    for y in range(4):
        mine, theirs = tab[SLOT + y], tab[SLOT + 4 + y]
        for k in range(2):
            o, r = own[mine, k], other[theirs, k]
            xs[:, 512 * y + 128 * k : 512 * y + 128 * k + 128] = jnp.where(first, o, r)
            xs[:, 512 * y + 256 + 128 * k : 512 * y + 384 + 128 * k] = jnp.where(first, r, o)
        for k in range(2):
            o, r = own[mine, 2 + k].astype(F32), other[theirs, 2 + k].astype(F32)
            e, f = jnp.where(first, o, r), jnp.where(first, r, o)
            low = jnp.concatenate([e[:, :64], f[:, :64]], axis=1)
            high = jnp.concatenate([e[:, 64:], f[:, 64:]], axis=1)
            pw[2 * k, :, 128 * y : 128 * y + 128] = low.astype(BF)
            pw[2 * k + 1, :, 128 * y : 128 * y + 128] = high.astype(BF)

    def norm(i, _):
        at = pl.ds(pl.multiple_of(i * 32, 32), 32)
        v = xs[at, :].astype(F32)
        scale = lax.rsqrt(jnp.mean(v * v, axis=1, keepdims=True) + EPS)
        n = (v * scale * gain_mix[...]).astype(BF)
        for j in range(4):
            ns[j, at, :] = n[:, 512 * j : 512 * j + 512]
        return 0

    lax.fori_loop(0, 16, norm, 0)

    def split(j, _):
        q = jnp.dot(ns[j], perm[...], preferred_element_type=F32).astype(BF)
        for g in range(4):
            ng[g, j] = q[:, 128 * g : 128 * g + 128]
        return 0

    lax.fori_loop(0, 4, split, 0)
    p = lax.broadcasted_iota(jnp.int32, (128, 128), 0)
    q = lax.broadcasted_iota(jnp.int32, (128, 128), 1)
    pos = lax.broadcasted_iota(jnp.int32, (128, 1), 0)
    for g in range(4):
        w = 2 ** (g + 1)
        window = jnp.where((q <= p) & (q > p - w), 1.0, 0.0).astype(BF)
        inverse = 1.0 / jnp.minimum(pos + 1, w).astype(F32)
        pieces = []
        for s in range(4):
            n = jnp.concatenate([ng[g, j, 128 * s : 128 * s + 128, :] for j in range(4)], axis=1)
            total = jnp.dot(window, n, preferred_element_type=F32)
            pieces.append((total * inverse - n.astype(F32)).astype(BF))
        pooled = jnp.concatenate(pieces, axis=0)
        m = jnp.dot(pooled, pw[g], preferred_element_type=F32)
        top = m.astype(BF)
        rest = (m - top.astype(F32)).astype(BF)
        for j in range(4):
            hi[j, :, 128 * g : 128 * g + 128] = top[:, 128 * j : 128 * j + 128]
            lo[j, :, 128 * g : 128 * g + 128] = rest[:, 128 * j : 128 * j + 128]

    for j in range(4):
        m = jnp.dot(hi[j], back[...], preferred_element_type=F32)
        m = m + jnp.dot(lo[j], back[...], preferred_element_type=F32)
        at = slice(512 * j, 512 * j + 512)
        xs[:, at] = (xs[:, at].astype(F32) + m * pool_gain[:, at]).astype(BF)

    def again(i, _):
        at = pl.ds(pl.multiple_of(i * 32, 32), 32)
        v = xs[at, :].astype(F32)
        scale = lax.rsqrt(jnp.mean(v * v, axis=1, keepdims=True) + EPS)
        out[at, :] = (v * scale * gain_ffn[...]).astype(BF)
        return 0

    lax.fori_loop(0, 16, again, 0)


def up_kernel(tab, x, gt, ut, g0, g1, g2, g3, u0, u1, u2, u3, h, ga, ua):
    for half, (refs, acc) in enumerate((((g0, g1, g2, g3), ga), ((u0, u1, u2, u3), ua))):
        for k, ref in enumerate(refs):
            cols = [
                x[:, pl.ds(pl.multiple_of(tab[16 * half + 4 * k + i] * 128, 128), 128)]
                for i in range(4)
            ]
            left = jnp.concatenate(cols, axis=1)
            right = jnp.concatenate([ref[i] for i in range(4)], axis=1)
            got = lax.dot_general(
                left, right, (((1,), (1,)), ((), ())), preferred_element_type=F32
            )
            acc[...] = got if k == 0 else acc[...] + got

    pos = lax.broadcasted_iota(jnp.int32, (LEN, 1), 0)

    def conv(v, taps):
        v = v.astype(BF).astype(F32)
        one = jnp.where(pos >= 1, pltpu.roll(v, 1, axis=0), 0.0)
        two = jnp.where(pos >= 2, pltpu.roll(v, 2, axis=0), 0.0)
        return two * taps[0:1, :] + one * taps[1:2, :] + v * taps[2:3, :]

    def finish(s, _):
        at = pl.ds(pl.multiple_of(s * LEN, LEN), LEN)
        for lo, hi in ((0, 256), (256, 512), (512, 704)):
            g = conv(ga[at, lo:hi], gt[:, lo:hi])
            u = conv(ua[at, lo:hi], ut[:, lo:hi])
            h[at, lo:hi] = (g / (1.0 + jnp.exp(-g)) * u).astype(BF)
        return 0

    lax.fori_loop(0, 4, finish, 0)


def down_kernel(tab, h, a0, a1, a2, a3, b0, b1, b2, b3, keep, give, acc):
    for half, refs in enumerate(((a0, a1, a2, a3), (b0, b1, b2, b3))):
        left = h[:, 0:384] if half == 0 else h[:, 384:704]
        for k, ref in enumerate(refs):
            right = jnp.concatenate([ref[i] for i in range(4)], axis=1)
            got = jnp.dot(left, right, preferred_element_type=F32)
            for i in range(4):
                at = tab[16 * half + 4 * k + i]
                piece = got[:, 128 * i : 128 * i + 128]
                acc[at] = piece if half == 0 else acc[at] + piece
    core = tab[CORE]
    for y in range(4):
        for i in range(2):
            keep[y, :, 128 * i : 128 * i + 128] = acc[4 * y + 2 * core + i]
            give[y, :, 128 * i : 128 * i + 128] = acc[4 * y + 2 * (1 - core) + i].astype(BF)


def add_four(tab, keep, got, give, rest):
    for i in range(2):
        at = tab[LAST + i]
        give[i] = (keep[at] + got[at].astype(F32)).astype(BF)
    for i in range(2):
        at = tab[LAST + 2 + i]
        rest[i] = keep[at] + got[at].astype(F32)


def add_two(keep, got, give, rest):
    rest[...] = keep[0] + got[0].astype(F32)
    give[...] = (keep[1] + got[1].astype(F32)).astype(BF)


def add_one(keep, got, out):
    out[...] = (keep[...] + got[...].astype(F32)).astype(BF)


def body(
    stream,
    gain_mix,
    pool_weight,
    pool_gain,
    gain_ffn,
    gate_weight,
    up_weight,
    gate_taps,
    up_taps,
    down_weight,
):
    fs, tp = lax.axis_index("fs"), lax.axis_index("tp")
    tab = lax.dynamic_index_in_dim(jnp.asarray(tables()), fs * 8 + tp, 0, keepdims=False)
    gt = lax.dynamic_slice_in_dim(gate_taps, tp * 704, 704, 1)
    ut = lax.dynamic_slice_in_dim(up_taps, tp * 704, 704, 1)

    a1, b1, spread = call(
        first_pack,
        "first_pack",
        [((1088, 128), BF), ((1024, 128), BF), ((16, 2, 32, 128), BF)],
        4,
    )(gate_weight.T, up_weight.T, down_weight, pool_weight)
    ra1, rb1 = send(a1, weight_perm(0, 0)), send(b1, weight_perm(1, 0))
    pool = lax.all_to_all(spread, "fs", split_axis=0, concat_axis=0, tiled=True)

    a2, b2 = call(
        pack_two, "pack_two", [((2, 1088, 128), BF), ((2, 1024, 128), BF)], 4
    )(a1, ra1, b1, rb1)
    ra2, rb2 = send(a2, weight_perm(0, 1)), send(b2, weight_perm(1, 1))

    (q1,) = call(column_pack, "column_pack", [((4, 512, 128), BF)], 2)(stream, pool)
    rq1 = send(q1, column_perm(0))

    ga, da, gb, db = call(
        pack_four,
        "pack_four",
        [((4, 704, 128), BF), ((4, 384, 128), BF), ((4, 704, 128), BF), ((4, 320, 128), BF)],
        4,
    )(a2, ra2, b2, rb2)
    third = weight_perm(0, 2), weight_perm(1, 2)
    fourth = weight_perm(0, 3), weight_perm(1, 3)
    rga, rgb = send(ga, third[0]), send(gb, third[1])
    rda, rdb = send(da, third[0]), send(db, third[1])

    (q2,) = call(column_two, "column_two", [((2, 4, 512, 128), BF)], 2)(q1, rq1)
    rq2 = send(q2, column_perm(1))

    sga, sgb = send(ga, fourth[0]), send(gb, fourth[1])
    (q4,) = call(column_four, "column_four", [((4, 4, 512, 128), BF)], 2)(q2, rq2)
    rq4 = send(q4, core_perm())

    srga, srgb = send(rga, fourth[0]), send(rgb, fourth[1])
    sda, sdb = send(da, fourth[0]), send(db, fourth[1])
    srda, srdb = send(rda, fourth[0]), send(rdb, fourth[1])

    (normed,) = call(
        mix_kernel,
        "mix",
        [((512, 2048), BF)],
        5,
        True,
        [
            pltpu.VMEM((512, 2048), BF),
            pltpu.VMEM((4, 512, 512), BF),
            pltpu.VMEM((4, 4, 512, 128), BF),
            pltpu.VMEM((4, 512, 512), BF),
            pltpu.VMEM((4, 512, 512), BF),
            pltpu.VMEM((4, 512, 512), BF),
            pltpu.VMEM((512, 512), BF),
            pltpu.VMEM((512, 512), BF),
        ],
        flops=6 * 10**9,
    )(tab, q4, rq4, gain_mix[None], pool_gain[None], gain_ffn[None])

    (hidden,) = call(
        up_kernel,
        "up",
        [((512, 704), BF)],
        11,
        True,
        [pltpu.VMEM((512, 704), F32), pltpu.VMEM((512, 704), F32)],
        flops=6 * 10**9,
    )(tab, normed, gt, ut, ga, rga, sga, srga, gb, rgb, sgb, srgb)

    keep4, give4 = call(
        down_kernel,
        "down",
        [((4, 512, 256), F32), ((4, 512, 256), BF)],
        9,
        True,
        [pltpu.VMEM((16, 512, 128), F32)],
        flops=2 * 10**9,
    )(tab, hidden, da, rda, sda, srda, db, rdb, sdb, srdb)
    got4 = send(give4, core_perm())
    give2, keep2 = call(
        add_four, "add_four", [((2, 512, 256), BF), ((2, 512, 256), F32)], 2, True
    )(tab, keep4, got4)
    got2 = send(give2, column_perm(0))
    give1, keep1 = call(add_two, "add_two", [((512, 256), BF), ((512, 256), F32)], 2)(
        keep2, got2
    )
    got1 = send(give1, column_perm(1))
    (out,) = call(add_one, "add_one", [((512, 256), BF)], 2)(keep1, got1)
    return out


def solution(mesh):
    return jax.shard_map(
        body,
        mesh=mesh,
        in_specs=(
            P("fs", "tp"),
            P(),
            P(None, "fs", "tp"),
            P(),
            P(),
            P("fs", "tp"),
            P("fs", "tp"),
            P(),
            P(),
            P("tp", "fs"),
        ),
        out_specs=P("fs", "tp"),
        check_vma=False,
    )
```
